32 devices in a mesh: row: 16 (over z, y, x), col: 2 (over core).
Axes of the slice: x: 2, y: 2, z: 4, core: 2. Of those that a mesh axis runs over, the one named last changes fastest.
Arguments:
- tokens: bfloat16 [2, 3072, 2048], P('col', 'row'), may hold values from -6 to 6
- proj_in: bfloat16 [2048, 512], P('col'), may hold values from -0.125 to 0.125
- proj_out: bfloat16 [512, 2048], P(None, 'row'), may hold values from -0.25 to 0.25
Outputs:
- output: bfloat16 [2, 3072, 2048], P('col', 'row')
The draws below stay inside these ranges and needn't reach their ends.
All inputs are finite; a program needn't handle non-finite values.
Results may differ from the reference program's by a relative error of at most 0.0083.
Values may be sent and summed in bfloat16 or wider, within the bound.
A program may use at most 64 MiB of HBM per device.

```python
import jax
import jax.numpy as jnp
from jax import lax

D = 2048
GROUPS = 4
GRP = 128
FW = 512
LEN = 3072
BATCH = 2


def steps_of(rng, extent, split, smallest, largest):
    level = 1.0
    for axis_at, shards_of in split:
        draws = jax.random.uniform(jax.random.fold_in(jax.random.fold_in(rng, 6), axis_at), (shards_of,), jnp.float32, smallest / len(split), largest / len(split))
        level = level * jnp.repeat(jnp.exp(draws), extent[axis_at] // shards_of).reshape((-1,) + (1,) * (len(extent) - 1 - axis_at))
    return level


def scatter_about(own_key, shape, spread, reach, pieces=(), kind=jnp.bfloat16):
    gain = steps_of(own_key, shape, pieces, -0.22, 0.18) if pieces else 1.0
    values = jax.random.normal(own_key, shape, jnp.float32) * spread * gain
    return jnp.minimum(jnp.maximum(values, -reach), reach).astype(kind)


def setup_inputs(seed: int = 0) -> dict:
    seeds = jax.random.split(jax.random.key(seed), 4)
    return {
        "tokens": scatter_about(seeds[0], (BATCH, LEN, D), 1.0, 6.0, ((0, 2), (1, 16))),
        "proj_in": scatter_about(seeds[1], (D, FW), D ** -0.5, 0.125, ((0, 2),)),
        "proj_out": scatter_about(seeds[2], (FW, D), FW ** -0.5, 0.25, ((1, 16),)),
    }


def reference(tokens, proj_in, proj_out):
    def one_sequence(seq):
        mapped = jnp.dot(seq, proj_in, preferred_element_type=jnp.float32).astype(jnp.bfloat16)
        length = seq.shape[0]
        grid = mapped.astype(jnp.float32).reshape(length, GROUPS, GRP)
        spectrum = jnp.fft.fft2(grid, axes=(0, 2), norm="ortho").real
        mixed = spectrum.reshape(length, GROUPS * GRP).astype(jnp.bfloat16)
        return jnp.dot(mixed, proj_out, preferred_element_type=jnp.float32).astype(jnp.bfloat16)

    return lax.map(one_sequence, tokens)
```

```python
import functools
import math

import jax
import jax.numpy as jnp
import numpy as np
from jax import lax
from jax.experimental import pallas as pl
from jax.experimental.pallas import tpu as pltpu
from jax.sharding import PartitionSpec as P

GRP = 128
LANES = 128
TILE = 16


highest = lax.Precision.HIGHEST
span_inner = 128


def circle(height, breadth, period):
    product = lax.iota(jnp.int32, height)[:, None] * lax.iota(jnp.int32, breadth)[None, :] % period
    angle = product.astype(jnp.float32) * (2.0 * math.pi / period)
    return (jnp.cos(angle), jnp.sin(angle))


def positions(piece):
    real_in = piece[0, 0]
    imag_in = piece[1, 0]
    count, length = real_in.shape
    outer = length // span_inner
    real_in = real_in.reshape(count, outer, span_inner)
    imag_in = imag_in.reshape(count, outer, span_inner)
    cos_one, sin_one = circle(outer, outer, outer)
    first_re = jnp.einsum("ab,kbq->kaq", cos_one, real_in, precision=highest) - jnp.einsum(
        "ab,kbq->kaq", sin_one, imag_in, precision=highest
    )
    first_im = jnp.einsum("ab,kbq->kaq", sin_one, real_in, precision=highest) + jnp.einsum(
        "ab,kbq->kaq", cos_one, imag_in, precision=highest
    )
    twist_c, twist_s = circle(outer, span_inner, length)
    turned_re = first_re * twist_c - first_im * twist_s
    turned_im = first_re * twist_s + first_im * twist_c
    cos_two, sin_two = circle(span_inner, span_inner, span_inner)
    factor = 1.0 / math.sqrt(GRP * length)
    real_out = jnp.einsum("kaq,qb->kba", turned_re, cos_two, precision=highest) - jnp.einsum(
        "kaq,qb->kba", turned_im, sin_two, precision=highest
    )
    real_out = real_out.reshape(count, length) * factor
    return real_out[:, None, :]


def plain(tokens, proj_in, proj_out):
    seq_rows = tokens[0]
    local_len = seq_rows.shape[0]
    features = proj_in.shape[1]
    groups = features // GRP
    mapped = jnp.dot(
        seq_rows,
        lax.all_gather(proj_in, "col", axis=0, tiled=True),
        preferred_element_type=jnp.float32,
    ).astype(jnp.bfloat16)
    values = mapped.astype(jnp.float32).reshape(local_len, groups, GRP)
    cos_c, sin_c = circle(GRP, GRP, GRP)
    real_part = jnp.einsum("pgc,cs->gsp", values, cos_c, precision=highest)
    imag_part = jnp.einsum("pgc,cs->gsp", values, sin_c, precision=highest)
    ways = lax.axis_size("row")
    slots = groups * cos_c.shape[1]
    per_dev = slots // ways
    stacked = jnp.stack(
        [real_part.reshape(ways, per_dev, local_len), imag_part.reshape(ways, per_dev, local_len)],
        0,
    )
    spectra = positions(lax.all_to_all(stacked, "row", split_axis=1, concat_axis=3, tiled=True))
    outgoing = spectra.astype(jnp.bfloat16)
    back = lax.all_to_all(outgoing, "row", split_axis=2, concat_axis=0, tiled=True)
    mixed = back.reshape(features, local_len)
    result = lax.dot_general(
        mixed,
        lax.all_gather(proj_out, "row", axis=1, tiled=True),
        (((0,), (0,)), ((), ())),
        preferred_element_type=jnp.float32,
    )
    return result.astype(jnp.bfloat16)[None]


def tables(ways, local_len, groups):
    slots = groups * GRP // ways
    half = slots // 2
    pack = LANES // slots
    rows = local_len // pack
    quads = ways // groups
    length = ways * local_len

    chan = np.arange(GRP)
    freq = np.arange(GRP // 2).reshape(quads, half)
    cos_part = np.cos(2 * np.pi * ((chan[:, None, None] * freq[None]) % GRP) / GRP)
    sin_part = np.sin(2 * np.pi * ((chan[:, None, None] * freq[None]) % GRP) / GRP)
    sin_part[:, 0, 0] = np.where(chan % 2 == 0, 1.0, -1.0)
    both = np.stack([cos_part, sin_part], 2).reshape(GRP, quads, 1, slots)
    spread = np.broadcast_to(both, (GRP, quads, pack, slots)).reshape(GRP, quads * LANES)

    joint = np.zeros((quads, 2, half, GRP))
    for quad in range(quads):
        for at in range(half):
            j = quad * half + at
            if j == 0:
                joint[quad, 0, at, 0] = 1.0
                joint[quad, 1, at, GRP // 2] = 1.0
            else:
                joint[quad, 0, at, j] = 1.0
                joint[quad, 1, at, j] = -1.0
                joint[quad, 0, at, GRP - j] = 1.0
                joint[quad, 1, at, GRP - j] = 1.0
    joint = joint.reshape(quads, 1, slots, GRP)
    gather = np.broadcast_to(joint, (quads, pack, slots, GRP)).reshape(quads * LANES, GRP)

    part = np.arange(pack)[:, None, None]
    dest = np.arange(ways)[None, :, None]
    sub = np.arange(rows // ways)[None, None, :]
    base = (dest * local_len + part * rows + sub * ways).reshape(-1, 1)
    q = np.arange(local_len)[None, :]
    factor = 1.0 / math.sqrt(GRP * length)
    pieces = []
    for a in range(ways // 2 + 1):
        angle = 2 * np.pi * ((base + a) * q % length) / length
        pieces.append(np.concatenate([np.cos(angle), -np.sin(angle)], 1))
        if 0 < a < ways // 2:
            angle = 2 * np.pi * ((base + ways - a) * q % length) / length
            pieces.append(np.concatenate([np.cos(angle), np.sin(angle)], 1))
    turn = np.concatenate(pieces, 0) * factor
    return tuple(t.astype(jnp.bfloat16) for t in (spread, gather, turn))


def scaled(x, factor):
    return x if abs(factor - 1.0) < 1e-12 else x * factor


def added(x, y):
    return y if x is None else x if y is None else x + y


def turned(re, im, cos, sin):
    def term(value, factor):
        return None if value is None or abs(factor) < 1e-12 else scaled(value, factor)

    return (added(term(re, cos), term(im, -sin)), added(term(re, sin), term(im, cos)))


def half_spectrum(xs):
    n = len(xs)
    if n == 1:
        return [(xs[0], None)]
    if n == 2:
        return [(xs[0] + xs[1], None), (xs[0] - xs[1], None)]
    even, odd = half_spectrum(xs[0::2]), half_spectrum(xs[1::2])
    out = [None] * (n // 2 + 1)
    for a in range(n // 4 + 1):
        er, ei = even[a]
        cos, sin = math.cos(2 * math.pi * a / n), math.sin(2 * math.pi * a / n)
        tr, ti = turned(*odd[a], cos, sin)
        minus = lambda v: None if v is None else -v
        out[a] = (added(er, tr), added(ei, ti))
        if n // 2 - a != a:
            out[n // 2 - a] = (added(er, minus(tr)), added(minus(ei), ti))
    return out


def flipped(index, bit):
    return index + bit - 2 * bit * ((index // bit) % 2)


def kernel(
    ways, cores, groups,
    tok_h, pin_h, pout_h, spread_h, gather_h, turn_h, out_h,
    tok, pin, wide, spread, gather, turn, acc, send1, recv1, spec, outer, send2, recv2, res,
    load_sem, out_sem, pin_send, pin_recv, ex_send, ex_recv, ag_send, ag_recv, fw_send, fw_recv,
):
    row = lax.axis_index("row")
    col = lax.axis_index("col")
    local_len = tok.shape[1]
    depth = pin_h.shape[0]
    features = pin_h.shape[1]
    width = pout_h.shape[1]
    slots = features // ways
    half = slots // 2
    pack = LANES // slots
    rows = local_len // pack
    quads = ways // groups
    share = features // cores

    def core(m):
        return lax.rem(col + m, cores)

    loads = []

    def load(src, dst):
        copy = pltpu.make_async_copy(src, dst, load_sem.at[len(loads)])
        copy.start()
        loads.append(copy)
        return copy

    def own_columns(index):
        return pl.ds(pl.multiple_of(index * width, LANES), width)

    first = [load(pin_h, pin.at[0])]
    for m in range(cores):
        at = pl.ds(pl.multiple_of(core(m) * depth, LANES), depth)
        copy = load(tok_h.at[0, :, at], tok.at[m])
        if m == 0:
            first.append(copy)
        else:
            later_tok = copy if m == 1 else later_tok
    rest_tok = loads[2:]
    own_out = load(pout_h, wide.at[:, own_columns(row)])
    load_spread = load(spread_h, spread)
    load_turn = load(turn_h, turn)
    load_gather = load(gather_h, gather)

    barrier = pltpu.get_barrier_semaphore()
    for m in range(1, ways):
        pl.semaphore_signal(barrier, inc=1, device_id={"row": lax.rem(row + m, ways)})
    for m in range(1, cores):
        pl.semaphore_signal(barrier, inc=1, device_id={"col": core(m)})

    for copy in first:
        copy.wait()
    acc[...] = jnp.dot(tok[0], pin[0], preferred_element_type=jnp.float32)
    own_out.wait()
    pl.semaphore_wait(barrier, ways - 1 + cores - 1)

    pin_copies = []
    for m in range(1, cores):
        copy = pltpu.make_async_remote_copy(
            pin.at[0], pin.at[cores - m], pin_send.at[m - 1], pin_recv.at[cores - m - 1],
            device_id={"col": core(m)},
        )
        copy.start()
        pin_copies.append(copy)

    bits = []
    bit = ways // 2
    while bit:
        bits.append(bit)
        bit //= 2
    if len(bits) >= 2:
        odd = lax.rem(col, 2)
        bits = bits[:-2] + [1 + odd, 2 - odd]
    blocks = [row]
    my_rows = pl.ds(pl.multiple_of(col * share, TILE), share)
    ag_copies = {}
    fw_copies = []

    def gather_step(step):
        for at in range(2**step):
            place = wide.at[my_rows, own_columns(blocks[at])]
            slot = at + 2**step
            copy = pltpu.make_async_remote_copy(
                place, place, ag_send.at[slot], ag_recv.at[slot],
                device_id={"row": flipped(row, bits[step])},
            )
            copy.start()
            ag_copies[slot] = copy
        blocks.extend([flipped(b, bits[step]) for b in blocks])

    def gather_land(step):
        for at in range(2**step, 2 ** (step + 1)):
            ag_copies[at].wait_recv()
            for m in range(1, cores):
                place = wide.at[my_rows, own_columns(blocks[at])]
                theirs = wide.at[
                    pl.ds(pl.multiple_of(core(m) * share, TILE), share), own_columns(blocks_of(m)[at])
                ]
                put = pltpu.make_async_remote_copy(
                    place, place, fw_send.at[at, m - 1], fw_recv.at[at, cores - m - 1],
                    device_id={"col": core(m)},
                )
                put.start()
                get = pltpu.make_async_remote_copy(
                    theirs, theirs, fw_send.at[at, m - 1], fw_recv.at[at, m - 1],
                    device_id={"col": core(m)},
                )
                fw_copies.append((put, get))

    def blocks_of(m):
        return blocks

    steps = len(bits)
    gather_step(0)

    for copy in rest_tok[: cores - 1]:
        copy.wait()
    total = acc[...]
    for m in range(1, cores):
        pin_copies[cores - 1 - m].wait_recv()
        total = total + jnp.dot(tok[m], pin[m], preferred_element_type=jnp.float32)
    mapped = total.astype(jnp.bfloat16)
    load_spread.wait()
    lane_part = lax.broadcasted_iota(jnp.int32, (GRP, quads * LANES), 1) // slots % pack
    table = spread[...]
    table = jnp.concatenate(
        [jnp.where(lane_part == t, table, jnp.zeros_like(table)) for t in range(pack)], 0
    )
    for g in range(groups):
        cut = mapped[:, g * GRP : (g + 1) * GRP]
        left = jnp.concatenate([cut[t * rows : (t + 1) * rows] for t in range(pack)], 1)
        made = jnp.dot(left, table, preferred_element_type=jnp.float32).astype(jnp.bfloat16)
        for quad in range(quads):
            send1[g * quads + quad] = made[:, quad * LANES : (quad + 1) * LANES]

    def exchange(src, dst, phase):
        copies = []
        for m in range(1, ways):
            to = lax.rem(row + m, ways)
            copy = pltpu.make_async_remote_copy(
                src.at[to], dst.at[row], ex_send.at[phase, m], ex_recv.at[phase, m],
                device_id={"row": to},
            )
            copy.start()
            copies.append(copy)
        dst[row] = src[row]
        return copies

    copies1 = exchange(send1, recv1, 0)
    for step in range(steps - 2):
        gather_land(step)
        gather_step(step + 1)
    for copy in copies1:
        copy.wait_recv()
    if steps >= 2:
        gather_land(steps - 2)
        gather_step(steps - 1)

    lane = lax.broadcasted_iota(jnp.int32, (1, LANES), 1) % slots
    lone = jnp.logical_and(lax.rem(row, quads) == 0, lane == half)
    sine = jnp.logical_and(lane >= half, jnp.logical_not(lone))
    sign = jnp.where(sine, -1.0, 1.0)
    for strip in range(rows // TILE):
        at = slice(strip * TILE, (strip + 1) * TILE)
        xs = [recv1[r, at, :].astype(jnp.float32) for r in range(ways)]
        for a, (re, im) in enumerate(half_spectrum(xs)):
            im = jnp.zeros_like(re) if im is None else im
            top = jnp.where(sine, im, re).astype(jnp.bfloat16)
            low = jnp.where(sine, -re, im).astype(jnp.bfloat16)
            for t in range(pack):
                begin = t * rows + strip * TILE
                spec[a, begin : begin + TILE, :] = top[:, t * slots : (t + 1) * slots]
                begin += local_len
                spec[a, begin : begin + TILE, :] = low[:, t * slots : (t + 1) * slots]
    load_turn.wait()
    begin = 0
    for a in range(ways // 2 + 1):
        single = a == 0 or 2 * a == ways
        size = local_len if single else 2 * local_len
        made = jnp.dot(turn[begin : begin + size], spec[a], preferred_element_type=jnp.float32)
        begin += size
        for at, which in enumerate([a] if single else [a, ways - a]):
            piece = jnp.concatenate(
                [made[at * local_len + t * rows : at * local_len + (t + 1) * rows] for t in range(pack)], 1
            )
            outer[pl.ds(which, rows, stride=ways), :] = piece if at == 0 else piece * sign
    for r in range(ways):
        send2[r] = outer[r * rows : (r + 1) * rows, :].astype(jnp.bfloat16)
    copies2 = exchange(send2, recv2, 1)

    load_gather.wait()
    row_part = lax.broadcasted_iota(jnp.int32, (quads * LANES, GRP), 0) // slots % pack
    table = gather[...]
    table = jnp.concatenate(
        [jnp.where(row_part == t, table, jnp.zeros_like(table)) for t in range(pack)], 1
    )
    for copy in copies2:
        copy.wait_recv()
    columns = []
    for g in range(groups):
        left = jnp.concatenate([recv2[g * quads + quad] for quad in range(quads)], 1)
        made = jnp.dot(left, table, preferred_element_type=jnp.float32).astype(jnp.bfloat16)
        columns.append(
            jnp.concatenate([made[:, t * GRP : (t + 1) * GRP] for t in range(pack)], 0)
        )
    mixed = jnp.concatenate(columns, 1)
    gather_land(steps - 1)
    for _, get in fw_copies:
        get.wait_recv()

    model = wide.shape[1]
    chunk = min(512, model)
    stores = []
    for at in range(model // chunk):
        span = slice(at * chunk, (at + 1) * chunk)
        res[:, span] = jnp.dot(mixed, wide[:, span], preferred_element_type=jnp.float32).astype(
            jnp.bfloat16
        )
        copy = pltpu.make_async_copy(res.at[:, span], out_h.at[0, :, span], out_sem.at[at])
        copy.start()
        stores.append(copy)
    for copy in copies1 + copies2 + pin_copies + list(ag_copies.values()):
        copy.wait_send()
    for put, _ in fw_copies:
        put.wait_send()
    for copy in stores:
        copy.wait()


def fused(ways, cores, tokens, proj_in, proj_out):
    _, local_len, model = tokens.shape
    depth, features = proj_in.shape
    width = proj_out.shape[1]
    groups = features // GRP
    slots = features // ways
    pack = LANES // slots
    rows = local_len // pack
    consts = [jnp.asarray(t) for t in tables(ways, local_len, groups)]
    bf, f32 = jnp.bfloat16, jnp.float32
    steps = ways
    dma = pltpu.SemaphoreType.DMA
    anywhere = pl.BlockSpec(memory_space=pl.ANY)
    return pl.pallas_call(
        functools.partial(kernel, ways, cores, groups),
        out_shape=jax.ShapeDtypeStruct(tokens.shape, bf),
        in_specs=[anywhere] * 6,
        out_specs=anywhere,
        scratch_shapes=[
            pltpu.VMEM((cores, local_len, depth), bf),
            pltpu.VMEM((cores, depth, features), bf),
            pltpu.VMEM((features, model), bf),
            pltpu.VMEM(consts[0].shape, bf),
            pltpu.VMEM(consts[1].shape, bf),
            pltpu.VMEM(consts[2].shape, bf),
            pltpu.VMEM((local_len, features), f32),
            pltpu.VMEM((ways, rows, LANES), bf),
            pltpu.VMEM((ways, rows, LANES), bf),
            pltpu.VMEM((ways // 2 + 1, 2 * local_len, slots), bf),
            pltpu.VMEM((ways * rows, LANES), f32),
            pltpu.VMEM((ways, rows, LANES), bf),
            pltpu.VMEM((ways, rows, LANES), bf),
            pltpu.VMEM((local_len, model), bf),
            dma((cores + 5,)),
            dma((max(1, model // 512),)),
            dma((cores,)),
            dma((cores,)),
            dma((2, ways)),
            dma((2, ways)),
            dma((ways,)),
            dma((ways,)),
            dma((ways, cores)),
            dma((ways, cores)),
        ],
        compiler_params=pltpu.CompilerParams(
            collective_id=0, has_side_effects=True, vmem_limit_bytes=48 * 2**20
        ),
    )(tokens, proj_in, proj_out, *consts)


def shards(ways, cores, tokens, proj_in, proj_out):
    _, local_len, model = tokens.shape
    depth, features = proj_in.shape
    width = proj_out.shape[1]
    groups = features // GRP
    slots = max(1, features // ways)
    pack = max(1, LANES // slots)
    fits = (
        ways >= 4
        and ways & (ways - 1) == 0
        and ways % groups == 0
        and slots * pack == LANES
        and slots % 2 == 0
        and cores == 2
        and local_len % pack == 0
        and (local_len // pack) % max(ways, TILE) == 0
        and width % LANES == 0
        and depth % LANES == 0
        and model % 512 == 0
        and features % (cores * TILE) == 0
    )
    if fits:
        return fused(ways, cores, tokens, proj_in, proj_out)
    return plain(tokens, proj_in, proj_out)


def solution(mesh):
    in_specs = (P("col", "row", None), P("col", None), P(None, "row"))
    out_specs = P("col", "row", None)
    body = functools.partial(shards, mesh.shape["row"], mesh.shape["col"])
    return jax.shard_map(body, mesh=mesh, in_specs=in_specs, out_specs=out_specs, check_vma=False)
```

```python
import functools
import math

import jax
import jax.numpy as jnp
import numpy as np
from jax import lax
from jax.experimental import pallas as pl
from jax.experimental.pallas import tpu as pltpu
from jax.sharding import PartitionSpec as P

GRP = 128
LANES = 128
TILE = 16


highest = lax.Precision.HIGHEST
span_inner = 128


def circle(height, breadth, period):
    product = lax.iota(jnp.int32, height)[:, None] * lax.iota(jnp.int32, breadth)[None, :] % period
    angle = product.astype(jnp.float32) * (2.0 * math.pi / period)
    return (jnp.cos(angle), jnp.sin(angle))


def positions(piece):
    real_in = piece[0, 0]
    imag_in = piece[1, 0]
    count, length = real_in.shape
    outer = length // span_inner
    real_in = real_in.reshape(count, outer, span_inner)
    imag_in = imag_in.reshape(count, outer, span_inner)
    cos_one, sin_one = circle(outer, outer, outer)
    first_re = jnp.einsum("ab,kbq->kaq", cos_one, real_in, precision=highest) - jnp.einsum(
        "ab,kbq->kaq", sin_one, imag_in, precision=highest
    )
    first_im = jnp.einsum("ab,kbq->kaq", sin_one, real_in, precision=highest) + jnp.einsum(
        "ab,kbq->kaq", cos_one, imag_in, precision=highest
    )
    twist_c, twist_s = circle(outer, span_inner, length)
    turned_re = first_re * twist_c - first_im * twist_s
    turned_im = first_re * twist_s + first_im * twist_c
    cos_two, sin_two = circle(span_inner, span_inner, span_inner)
    factor = 1.0 / math.sqrt(GRP * length)
    real_out = jnp.einsum("kaq,qb->kba", turned_re, cos_two, precision=highest) - jnp.einsum(
        "kaq,qb->kba", turned_im, sin_two, precision=highest
    )
    real_out = real_out.reshape(count, length) * factor
    return real_out[:, None, :]


def plain(tokens, proj_in, proj_out):
    seq_rows = tokens[0]
    local_len = seq_rows.shape[0]
    features = proj_in.shape[1]
    groups = features // GRP
    mapped = jnp.dot(
        seq_rows,
        lax.all_gather(proj_in, "col", axis=0, tiled=True),
        preferred_element_type=jnp.float32,
    ).astype(jnp.bfloat16)
    values = mapped.astype(jnp.float32).reshape(local_len, groups, GRP)
    cos_c, sin_c = circle(GRP, GRP, GRP)
    real_part = jnp.einsum("pgc,cs->gsp", values, cos_c, precision=highest)
    imag_part = jnp.einsum("pgc,cs->gsp", values, sin_c, precision=highest)
    ways = lax.axis_size("row")
    slots = groups * cos_c.shape[1]
    per_dev = slots // ways
    stacked = jnp.stack(
        [real_part.reshape(ways, per_dev, local_len), imag_part.reshape(ways, per_dev, local_len)],
        0,
    )
    spectra = positions(lax.all_to_all(stacked, "row", split_axis=1, concat_axis=3, tiled=True))
    outgoing = spectra.astype(jnp.bfloat16)
    back = lax.all_to_all(outgoing, "row", split_axis=2, concat_axis=0, tiled=True)
    mixed = back.reshape(features, local_len)
    result = lax.dot_general(
        mixed,
        lax.all_gather(proj_out, "row", axis=1, tiled=True),
        (((0,), (0,)), ((), ())),
        preferred_element_type=jnp.float32,
    )
    return result.astype(jnp.bfloat16)[None]


def tables(ways, local_len, groups):
    slots = groups * GRP // ways
    half = slots // 2
    pack = LANES // slots
    rows = local_len // pack
    quads = ways // groups
    length = ways * local_len

    chan = np.arange(GRP)
    freq = np.arange(GRP // 2).reshape(quads, half)
    cos_part = np.cos(2 * np.pi * ((chan[:, None, None] * freq[None]) % GRP) / GRP)
    sin_part = np.sin(2 * np.pi * ((chan[:, None, None] * freq[None]) % GRP) / GRP)
    sin_part[:, 0, 0] = np.where(chan % 2 == 0, 1.0, -1.0)
    both = np.stack([cos_part, sin_part], 2).reshape(GRP, quads, 1, slots)
    spread = np.broadcast_to(both, (GRP, quads, pack, slots)).reshape(GRP, quads * LANES)

    joint = np.zeros((quads, 2, half, GRP))
    for quad in range(quads):
        for at in range(half):
            j = quad * half + at
            if j == 0:
                joint[quad, 0, at, 0] = 1.0
                joint[quad, 1, at, GRP // 2] = 1.0
            else:
                joint[quad, 0, at, j] = 1.0
                joint[quad, 1, at, j] = -1.0
                joint[quad, 0, at, GRP - j] = 1.0
                joint[quad, 1, at, GRP - j] = 1.0
    joint = joint.reshape(quads, 1, slots, GRP)
    gather = np.broadcast_to(joint, (quads, pack, slots, GRP)).reshape(quads * LANES, GRP)

    part = np.arange(pack)[:, None, None]
    dest = np.arange(ways)[None, :, None]
    sub = np.arange(rows // ways)[None, None, :]
    base = (dest * local_len + part * rows + sub * ways).reshape(-1, 1)
    q = np.arange(local_len)[None, :]
    factor = 1.0 / math.sqrt(GRP * length)
    pieces = []
    for a in range(ways // 2 + 1):
        angle = 2 * np.pi * ((base + a) * q % length) / length
        pieces.append(np.concatenate([np.cos(angle), -np.sin(angle)], 1))
        if 0 < a < ways // 2:
            angle = 2 * np.pi * ((base + ways - a) * q % length) / length
            pieces.append(np.concatenate([np.cos(angle), np.sin(angle)], 1))
    turn = np.concatenate(pieces, 0) * factor
    return tuple(t.astype(jnp.bfloat16) for t in (spread, gather, turn))


def scaled(x, factor):
    return x if abs(factor - 1.0) < 1e-12 else x * factor


def added(x, y):
    return y if x is None else x if y is None else x + y


def turned(re, im, cos, sin):
    def term(value, factor):
        return None if value is None or abs(factor) < 1e-12 else scaled(value, factor)

    return (added(term(re, cos), term(im, -sin)), added(term(re, sin), term(im, cos)))


def half_spectrum(xs):
    n = len(xs)
    if n == 1:
        return [(xs[0], None)]
    if n == 2:
        return [(xs[0] + xs[1], None), (xs[0] - xs[1], None)]
    even, odd = half_spectrum(xs[0::2]), half_spectrum(xs[1::2])
    out = [None] * (n // 2 + 1)
    for a in range(n // 4 + 1):
        er, ei = even[a]
        cos, sin = math.cos(2 * math.pi * a / n), math.sin(2 * math.pi * a / n)
        tr, ti = turned(*odd[a], cos, sin)
        minus = lambda v: None if v is None else -v
        out[a] = (added(er, tr), added(ei, ti))
        if n // 2 - a != a:
            out[n // 2 - a] = (added(er, minus(tr)), added(minus(ei), ti))
    return out


def flipped(index, bit):
    return index + bit - 2 * bit * ((index // bit) % 2)


def kernel(
    ways, cores, groups,
    tok_h, pin_h, pout_h, spread_h, gather_h, turn_h, out_h,
    tok, pin, wide, spread, gather, turn, acc, send1, recv1, spec, outer, send2, recv2, res,
    load_sem, out_sem, pin_send, pin_recv, ex_send, ex_recv, ag_send, ag_recv, fw_send, fw_recv,
):
    row = lax.axis_index("row")
    col = lax.axis_index("col")
    local_len = tok.shape[1]
    depth = pin_h.shape[0]
    features = pin_h.shape[1]
    width = pout_h.shape[1]
    slots = features // ways
    half = slots // 2
    pack = LANES // slots
    rows = local_len // pack
    quads = ways // groups
    share = features // cores

    def core(m):
        return lax.rem(col + m, cores)

    loads = []

    def load(src, dst):
        copy = pltpu.make_async_copy(src, dst, load_sem.at[len(loads)])
        copy.start()
        loads.append(copy)
        return copy

    def own_columns(index):
        return pl.ds(pl.multiple_of(index * width, LANES), width)

    first = [load(pin_h, pin.at[0])]
    for m in range(cores):
        at = pl.ds(pl.multiple_of(core(m) * depth, LANES), depth)
        copy = load(tok_h.at[0, :, at], tok.at[m])
        if m == 0:
            first.append(copy)
    rest_tok = loads[2:]
    own_out = load(pout_h, wide.at[:, own_columns(row)])
    load_spread = load(spread_h, spread)
    load_turn = load(turn_h, turn)
    load_gather = load(gather_h, gather)

    barrier = pltpu.get_barrier_semaphore()
    for m in range(1, ways):
        pl.semaphore_signal(barrier, inc=1, device_id={"row": lax.rem(row + m, ways)})
    for m in range(1, cores):
        pl.semaphore_signal(barrier, inc=1, device_id={"col": core(m)})

    for copy in first:
        copy.wait()
    acc[...] = jnp.dot(tok[0], pin[0], preferred_element_type=jnp.float32)
    own_out.wait()
    pl.semaphore_wait(barrier, ways - 1 + cores - 1)

    pin_copies = []
    for m in range(1, cores):
        copy = pltpu.make_async_remote_copy(
            pin.at[0], pin.at[cores - m], pin_send.at[m - 1], pin_recv.at[cores - m - 1],
            device_id={"col": core(m)},
        )
        copy.start()
        pin_copies.append(copy)

    bits = []
    bit = ways // 2
    while bit:
        bits.append(bit)
        bit //= 2
    if len(bits) >= 2:
        odd = lax.rem(col, 2)
        bits = bits[:-2] + [1 + odd, 2 - odd]
    steps = len(bits)
    blocks = [row]
    for bit in bits:
        blocks = blocks + [flipped(b, bit) for b in blocks]
    my_rows = pl.ds(pl.multiple_of(col * share, TILE), share)
    ag_copies = {}
    fw_copies = []

    def land(at):
        ag_copies[at].wait_recv()
        for m in range(1, cores):
            theirs = pl.ds(pl.multiple_of(core(m) * share, TILE), share)
            ours = wide.at[my_rows, own_columns(blocks[at])]
            other = wide.at[theirs, own_columns(blocks[at])]
            put = pltpu.make_async_remote_copy(
                ours, ours, fw_send.at[at, m - 1], fw_recv.at[at, cores - m - 1],
                device_id={"col": core(m)},
            )
            put.start()
            get = pltpu.make_async_remote_copy(
                other, other, fw_send.at[at, m - 1], fw_recv.at[at, m - 1],
                device_id={"col": core(m)},
            )
            fw_copies.append((put, get))

    def level(count):
        for at in range(ways):
            if at.bit_count() != count:
                continue
            if count:
                land(at)
            for step in range(at.bit_length(), steps):
                place = wide.at[my_rows, own_columns(blocks[at])]
                slot = at + 2**step
                copy = pltpu.make_async_remote_copy(
                    place, place, ag_send.at[slot], ag_recv.at[slot],
                    device_id={"row": flipped(row, bits[step])},
                )
                copy.start()
                ag_copies[slot] = copy

    level(0)

    for copy in rest_tok[: cores - 1]:
        copy.wait()
    total = acc[...]
    for m in range(1, cores):
        pin_copies[cores - 1 - m].wait_recv()
        total = total + jnp.dot(tok[m], pin[m], preferred_element_type=jnp.float32)
    mapped = total.astype(jnp.bfloat16)
    load_spread.wait()
    lane_part = lax.broadcasted_iota(jnp.int32, (GRP, quads * LANES), 1) // slots % pack
    table = spread[...]
    table = jnp.concatenate(
        [jnp.where(lane_part == t, table, jnp.zeros_like(table)) for t in range(pack)], 0
    )
    for g in range(groups):
        cut = mapped[:, g * GRP : (g + 1) * GRP]
        left = jnp.concatenate([cut[t * rows : (t + 1) * rows] for t in range(pack)], 1)
        made = jnp.dot(left, table, preferred_element_type=jnp.float32).astype(jnp.bfloat16)
        for quad in range(quads):
            send1[g * quads + quad] = made[:, quad * LANES : (quad + 1) * LANES]

    def exchange(src, dst, phase):
        copies = []
        for m in range(1, ways):
            to = lax.rem(row + m, ways)
            copy = pltpu.make_async_remote_copy(
                src.at[to], dst.at[row], ex_send.at[phase, m], ex_recv.at[phase, m],
                device_id={"row": to},
            )
            copy.start()
            copies.append(copy)
        dst[row] = src[row]
        return copies

    copies1 = exchange(send1, recv1, 0)
    level(1)
    for copy in copies1:
        copy.wait_recv()
    level(2)

    lane = lax.broadcasted_iota(jnp.int32, (1, LANES), 1) % slots
    lone = jnp.logical_and(lax.rem(row, quads) == 0, lane == half)
    sine = jnp.logical_and(lane >= half, jnp.logical_not(lone))
    sign = jnp.where(sine, -1.0, 1.0)
    for strip in range(rows // TILE):
        at = slice(strip * TILE, (strip + 1) * TILE)
        xs = [recv1[r, at, :].astype(jnp.float32) for r in range(ways)]
        for a, (re, im) in enumerate(half_spectrum(xs)):
            im = jnp.zeros_like(re) if im is None else im
            top = jnp.where(sine, im, re).astype(jnp.bfloat16)
            low = jnp.where(sine, -re, im).astype(jnp.bfloat16)
            for t in range(pack):
                begin = t * rows + strip * TILE
                spec[a, begin : begin + TILE, :] = top[:, t * slots : (t + 1) * slots]
                begin += local_len
                spec[a, begin : begin + TILE, :] = low[:, t * slots : (t + 1) * slots]
    load_turn.wait()
    begin = 0
    for a in range(ways // 2 + 1):
        single = a == 0 or 2 * a == ways
        size = local_len if single else 2 * local_len
        made = jnp.dot(turn[begin : begin + size], spec[a], preferred_element_type=jnp.float32)
        begin += size
        for at, which in enumerate([a] if single else [a, ways - a]):
            piece = jnp.concatenate(
                [made[at * local_len + t * rows : at * local_len + (t + 1) * rows] for t in range(pack)], 1
            )
            outer[pl.ds(which, rows, stride=ways), :] = piece if at == 0 else piece * sign
    for r in range(ways):
        send2[r] = outer[r * rows : (r + 1) * rows, :].astype(jnp.bfloat16)
    copies2 = exchange(send2, recv2, 1)
    for count in range(3, steps):
        level(count)

    load_gather.wait()
    row_part = lax.broadcasted_iota(jnp.int32, (quads * LANES, GRP), 0) // slots % pack
    table = gather[...]
    table = jnp.concatenate(
        [jnp.where(row_part == t, table, jnp.zeros_like(table)) for t in range(pack)], 1
    )
    for copy in copies2:
        copy.wait_recv()
    columns = []
    for g in range(groups):
        left = jnp.concatenate([recv2[g * quads + quad] for quad in range(quads)], 1)
        made = jnp.dot(left, table, preferred_element_type=jnp.float32).astype(jnp.bfloat16)
        columns.append(
            jnp.concatenate([made[:, t * GRP : (t + 1) * GRP] for t in range(pack)], 0)
        )
    mixed = jnp.concatenate(columns, 1)
    level(steps)
    for _, get in fw_copies:
        get.wait_recv()

    model = wide.shape[1]
    chunk = min(512, model)
    stores = []
    for at in range(model // chunk):
        span = slice(at * chunk, (at + 1) * chunk)
        res[:, span] = jnp.dot(mixed, wide[:, span], preferred_element_type=jnp.float32).astype(
            jnp.bfloat16
        )
        copy = pltpu.make_async_copy(res.at[:, span], out_h.at[0, :, span], out_sem.at[at])
        copy.start()
        stores.append(copy)
    for copy in copies1 + copies2 + pin_copies + list(ag_copies.values()):
        copy.wait_send()
    for put, _ in fw_copies:
        put.wait_send()
    for copy in stores:
        copy.wait()


def fused(ways, cores, tokens, proj_in, proj_out):
    _, local_len, model = tokens.shape
    depth, features = proj_in.shape
    width = proj_out.shape[1]
    groups = features // GRP
    slots = features // ways
    pack = LANES // slots
    rows = local_len // pack
    consts = [jnp.asarray(t) for t in tables(ways, local_len, groups)]
    bf, f32 = jnp.bfloat16, jnp.float32
    dma = pltpu.SemaphoreType.DMA
    anywhere = pl.BlockSpec(memory_space=pltpu.HBM)
    return pl.pallas_call(
        functools.partial(kernel, ways, cores, groups),
        out_shape=jax.ShapeDtypeStruct(tokens.shape, bf),
        in_specs=[anywhere] * 6,
        out_specs=anywhere,
        scratch_shapes=[
            pltpu.VMEM((cores, local_len, depth), bf),
            pltpu.VMEM((cores, depth, features), bf),
            pltpu.VMEM((features, model), bf),
            pltpu.VMEM(consts[0].shape, bf),
            pltpu.VMEM(consts[1].shape, bf),
            pltpu.VMEM(consts[2].shape, bf),
            pltpu.VMEM((local_len, features), f32),
            pltpu.VMEM((ways, rows, LANES), bf),
            pltpu.VMEM((ways, rows, LANES), bf),
            pltpu.VMEM((ways // 2 + 1, 2 * local_len, slots), bf),
            pltpu.VMEM((ways * rows, LANES), f32),
            pltpu.VMEM((ways, rows, LANES), bf),
            pltpu.VMEM((ways, rows, LANES), bf),
            pltpu.VMEM((local_len, model), bf),
            dma((cores + 5,)),
            dma((max(1, model // 512),)),
            dma((cores,)),
            dma((cores,)),
            dma((2, ways)),
            dma((2, ways)),
            dma((ways,)),
            dma((ways,)),
            dma((ways, cores)),
            dma((ways, cores)),
        ],
        compiler_params=pltpu.CompilerParams(
            collective_id=0, has_side_effects=True, vmem_limit_bytes=67043328
        ),
    )(tokens, proj_in, proj_out, *consts)


def shards(ways, cores, tokens, proj_in, proj_out):
    _, local_len, model = tokens.shape
    depth, features = proj_in.shape
    width = proj_out.shape[1]
    groups = features // GRP
    slots = max(1, features // ways)
    pack = max(1, LANES // slots)
    fits = (
        ways >= 4
        and ways & (ways - 1) == 0
        and ways % groups == 0
        and slots * pack == LANES
        and slots % 2 == 0
        and cores == 2
        and local_len % pack == 0
        and (local_len // pack) % max(ways, TILE) == 0
        and width % LANES == 0
        and depth % LANES == 0
        and model % 512 == 0
        and features % (cores * TILE) == 0
    )
    if fits:
        return fused(ways, cores, tokens, proj_in, proj_out)
    return plain(tokens, proj_in, proj_out)


def solution(mesh):
    in_specs = (P("col", "row", None), P("col", None), P(None, "row"))
    out_specs = P("col", "row", None)
    body = functools.partial(shards, mesh.shape["row"], mesh.shape["col"])
    return jax.shard_map(body, mesh=mesh, in_specs=in_specs, out_specs=out_specs, check_vma=False)
```

```python
import functools
import math

import jax
import jax.numpy as jnp
import numpy as np
from jax import lax
from jax.experimental import pallas as pl
from jax.experimental.pallas import tpu as pltpu
from jax.sharding import PartitionSpec as P

GRP = 128
LANES = 128
TILE = 16
PARTS = 4


highest = lax.Precision.HIGHEST
span_inner = 128


def circle(height, breadth, period):
    product = lax.iota(jnp.int32, height)[:, None] * lax.iota(jnp.int32, breadth)[None, :] % period
    angle = product.astype(jnp.float32) * (2.0 * math.pi / period)
    return (jnp.cos(angle), jnp.sin(angle))


def positions(piece):
    real_in = piece[0, 0]
    imag_in = piece[1, 0]
    count, length = real_in.shape
    outer = length // span_inner
    real_in = real_in.reshape(count, outer, span_inner)
    imag_in = imag_in.reshape(count, outer, span_inner)
    cos_one, sin_one = circle(outer, outer, outer)
    first_re = jnp.einsum("ab,kbq->kaq", cos_one, real_in, precision=highest) - jnp.einsum(
        "ab,kbq->kaq", sin_one, imag_in, precision=highest
    )
    first_im = jnp.einsum("ab,kbq->kaq", sin_one, real_in, precision=highest) + jnp.einsum(
        "ab,kbq->kaq", cos_one, imag_in, precision=highest
    )
    twist_c, twist_s = circle(outer, span_inner, length)
    turned_re = first_re * twist_c - first_im * twist_s
    turned_im = first_re * twist_s + first_im * twist_c
    cos_two, sin_two = circle(span_inner, span_inner, span_inner)
    factor = 1.0 / math.sqrt(GRP * length)
    real_out = jnp.einsum("kaq,qb->kba", turned_re, cos_two, precision=highest) - jnp.einsum(
        "kaq,qb->kba", turned_im, sin_two, precision=highest
    )
    real_out = real_out.reshape(count, length) * factor
    return real_out[:, None, :]


def plain(tokens, proj_in, proj_out):
    seq_rows = tokens[0]
    local_len = seq_rows.shape[0]
    features = proj_in.shape[1]
    groups = features // GRP
    mapped = jnp.dot(
        seq_rows,
        lax.all_gather(proj_in, "col", axis=0, tiled=True),
        preferred_element_type=jnp.float32,
    ).astype(jnp.bfloat16)
    values = mapped.astype(jnp.float32).reshape(local_len, groups, GRP)
    cos_c, sin_c = circle(GRP, GRP, GRP)
    real_part = jnp.einsum("pgc,cs->gsp", values, cos_c, precision=highest)
    imag_part = jnp.einsum("pgc,cs->gsp", values, sin_c, precision=highest)
    ways = lax.axis_size("row")
    slots = groups * cos_c.shape[1]
    per_dev = slots // ways
    stacked = jnp.stack(
        [real_part.reshape(ways, per_dev, local_len), imag_part.reshape(ways, per_dev, local_len)],
        0,
    )
    spectra = positions(lax.all_to_all(stacked, "row", split_axis=1, concat_axis=3, tiled=True))
    outgoing = spectra.astype(jnp.bfloat16)
    back = lax.all_to_all(outgoing, "row", split_axis=2, concat_axis=0, tiled=True)
    mixed = back.reshape(features, local_len)
    result = lax.dot_general(
        mixed,
        lax.all_gather(proj_out, "row", axis=1, tiled=True),
        (((0,), (0,)), ((), ())),
        preferred_element_type=jnp.float32,
    )
    return result.astype(jnp.bfloat16)[None]


def tables(ways, local_len, groups):
    slots = groups * GRP // ways
    half = slots // 2
    pack = LANES // slots
    rows = local_len // pack
    quads = ways // groups
    length = ways * local_len

    chan = np.arange(GRP)
    freq = np.arange(GRP // 2).reshape(quads, half)
    cos_part = np.cos(2 * np.pi * ((chan[:, None, None] * freq[None]) % GRP) / GRP)
    sin_part = np.sin(2 * np.pi * ((chan[:, None, None] * freq[None]) % GRP) / GRP)
    sin_part[:, 0, 0] = np.where(chan % 2 == 0, 1.0, -1.0)
    both = np.stack([cos_part, sin_part], 2).reshape(GRP, quads, 1, slots)
    spread = np.broadcast_to(both, (GRP, quads, pack, slots)).reshape(GRP, quads * LANES)

    joint = np.zeros((quads, 2, half, GRP))
    for quad in range(quads):
        for at in range(half):
            j = quad * half + at
            if j == 0:
                joint[quad, 0, at, 0] = 1.0
                joint[quad, 1, at, GRP // 2] = 1.0
            else:
                joint[quad, 0, at, j] = 1.0
                joint[quad, 1, at, j] = -1.0
                joint[quad, 0, at, GRP - j] = 1.0
                joint[quad, 1, at, GRP - j] = 1.0
    joint = joint.reshape(quads, 1, slots, GRP)
    gather = np.broadcast_to(joint, (quads, pack, slots, GRP)).reshape(quads * LANES, GRP)

    part = np.arange(pack)[:, None, None]
    dest = np.arange(ways)[None, :, None]
    sub = np.arange(rows // ways)[None, None, :]
    base = (dest * local_len + part * rows + sub * ways).reshape(-1, 1)
    q = np.arange(local_len)[None, :]
    factor = 1.0 / math.sqrt(GRP * length)
    pieces = []
    for a in range(ways // 2 + 1):
        angle = 2 * np.pi * ((base + a) * q % length) / length
        pieces.append(np.concatenate([np.cos(angle), -np.sin(angle)], 1))
        if 0 < a < ways // 2:
            angle = 2 * np.pi * ((base + ways - a) * q % length) / length
            pieces.append(np.concatenate([np.cos(angle), np.sin(angle)], 1))
    turn = np.concatenate(pieces, 0) * factor
    return tuple(t.astype(jnp.bfloat16) for t in (spread, gather, turn))


def scaled(x, factor):
    return x if abs(factor - 1.0) < 1e-12 else x * factor


def added(x, y):
    return y if x is None else x if y is None else x + y


def turned(re, im, cos, sin):
    def term(value, factor):
        return None if value is None or abs(factor) < 1e-12 else scaled(value, factor)

    return (added(term(re, cos), term(im, -sin)), added(term(re, sin), term(im, cos)))


def half_spectrum(xs):
    n = len(xs)
    if n == 1:
        return [(xs[0], None)]
    if n == 2:
        return [(xs[0] + xs[1], None), (xs[0] - xs[1], None)]
    even, odd = half_spectrum(xs[0::2]), half_spectrum(xs[1::2])
    out = [None] * (n // 2 + 1)
    for a in range(n // 4 + 1):
        er, ei = even[a]
        cos, sin = math.cos(2 * math.pi * a / n), math.sin(2 * math.pi * a / n)
        tr, ti = turned(*odd[a], cos, sin)
        minus = lambda v: None if v is None else -v
        out[a] = (added(er, tr), added(ei, ti))
        if n // 2 - a != a:
            out[n // 2 - a] = (added(er, minus(tr)), added(minus(ei), ti))
    return out


def flipped(index, bit):
    return index + bit - 2 * bit * ((index // bit) % 2)


def partners(index, ways):
    return [(m, lax.rem(index + m, ways)) for m in range(1, ways)]


def kernel(
    ways, cores, groups,
    tok_h, pin_h, pout_h, spread_h, gather_h, turn_h, mixed_v, wide,
    tok, pin, spread, gather, turn, acc, send1, recv1, spec, outer, send2, recv2,
    load_sem, pin_send, pin_recv, ex_send, ex_recv, ag_send, ag_recv, fw_send, fw_recv,
):
    row = lax.axis_index("row")
    col = lax.axis_index("col")
    local_len = tok.shape[1]
    depth = pin_h.shape[0]
    features = pin_h.shape[1]
    width = pout_h.shape[1]
    slots = features // ways
    half = slots // 2
    pack = LANES // slots
    rows = local_len // pack
    quads = ways // groups
    share = features // cores

    def core(m):
        return lax.rem(col + m, cores)

    peers = partners(row, ways)
    barrier = pltpu.get_barrier_semaphore()
    for _, to in peers:
        pl.semaphore_signal(barrier, inc=1, device_id={"row": to})
    for m in range(1, cores):
        pl.semaphore_signal(barrier, inc=1, device_id={"col": core(m)})

    loads = []

    def load(src, dst):
        copy = pltpu.make_async_copy(src, dst, load_sem.at[len(loads)])
        copy.start()
        loads.append(copy)
        return copy

    def own_columns(index):
        return pl.ds(pl.multiple_of(index * width, LANES), width)

    first = [load(pin_h, pin.at[0])]
    for m in range(cores):
        at = pl.ds(pl.multiple_of(core(m) * depth, LANES), depth)
        copy = load(tok_h.at[0, :, at], tok.at[m])
        if m == 0:
            first.append(copy)
    rest_tok = loads[2:]
    own_out = load(pout_h, wide.at[:, own_columns(row)])
    load_spread = load(spread_h, spread)
    load_turn = load(turn_h, turn)
    load_gather = load(gather_h, gather)

    for copy in first:
        copy.wait()
    acc[...] = jnp.dot(tok[0], pin[0], preferred_element_type=jnp.float32)
    own_out.wait()
    pl.semaphore_wait(barrier, ways - 1 + cores - 1)

    pin_copies = []
    part = depth // PARTS
    for m in range(1, cores):
        for at in range(PARTS):
            span = pl.ds(at * part, part)
            copy = pltpu.make_async_remote_copy(
                pin.at[0, span], pin.at[cores - m, span],
                pin_send.at[m - 1, at], pin_recv.at[cores - m - 1, at],
                device_id={"col": core(m)},
            )
            copy.start()
            pin_copies.append(copy)

    bits = []
    bit = ways // 2
    while bit:
        bits.append(bit)
        bit //= 2
    if len(bits) >= 2:
        odd = lax.rem(col, 2)
        bits = bits[:-2] + [1 + odd, 2 - odd]
    steps = len(bits)
    blocks = [row]
    for bit in bits:
        blocks = blocks + [flipped(b, bit) for b in blocks]
    my_rows = pl.ds(pl.multiple_of(col * share, TILE), share)
    ag_copies = {}
    fw_copies = []

    def land(at):
        ag_copies[at].wait_recv()
        for m in range(1, cores):
            theirs = pl.ds(pl.multiple_of(core(m) * share, TILE), share)
            ours = wide.at[my_rows, own_columns(blocks[at])]
            other = wide.at[theirs, own_columns(blocks[at])]
            put = pltpu.make_async_remote_copy(
                ours, ours, fw_send.at[at, m - 1], fw_recv.at[at, cores - m - 1],
                device_id={"col": core(m)},
            )
            put.start()
            get = pltpu.make_async_remote_copy(
                other, other, fw_send.at[at, m - 1], fw_recv.at[at, m - 1],
                device_id={"col": core(m)},
            )
            fw_copies.append((put, get))

    def level(count):
        for at in range(ways):
            if at.bit_count() != count:
                continue
            if count:
                land(at)
            for step in range(at.bit_length(), steps):
                place = wide.at[my_rows, own_columns(blocks[at])]
                slot = at + 2**step
                copy = pltpu.make_async_remote_copy(
                    place, place, ag_send.at[slot], ag_recv.at[slot],
                    device_id={"row": flipped(row, bits[step])},
                )
                copy.start()
                ag_copies[slot] = copy

    level(0)

    for copy in rest_tok[: cores - 1]:
        copy.wait()
    total = acc[...]
    for m in range(1, cores):
        for at in range(PARTS):
            span = slice(at * part, (at + 1) * part)
            pin_copies[(cores - 1 - m) * PARTS + at].wait_recv()
            total = total + jnp.dot(tok[m, :, span], pin[m, span], preferred_element_type=jnp.float32)
    mapped = total.astype(jnp.bfloat16)
    load_spread.wait()
    lane_part = lax.broadcasted_iota(jnp.int32, (GRP, quads * LANES), 1) // slots % pack
    table = spread[...]
    table = jnp.concatenate(
        [jnp.where(lane_part == t, table, jnp.zeros_like(table)) for t in range(pack)], 0
    )
    for g in range(groups):
        cut = mapped[:, g * GRP : (g + 1) * GRP]
        left = jnp.concatenate([cut[t * rows : (t + 1) * rows] for t in range(pack)], 1)
        made = jnp.dot(left, table, preferred_element_type=jnp.float32).astype(jnp.bfloat16)
        for quad in range(quads):
            send1[g * quads + quad] = made[:, quad * LANES : (quad + 1) * LANES]

    def exchange(src, dst, phase):
        copies = []
        for m, to in peers:
            copy = pltpu.make_async_remote_copy(
                src.at[to], dst.at[row], ex_send.at[phase, m], ex_recv.at[phase, m],
                device_id={"row": to},
            )
            copy.start()
            copies.append(copy)
        dst[row] = src[row]
        return copies

    copies1 = exchange(send1, recv1, 0)
    level(1)
    for copy in copies1:
        copy.wait_recv()
    level(2)

    lane = lax.broadcasted_iota(jnp.int32, (1, LANES), 1) % slots
    lone = jnp.logical_and(lax.rem(row, quads) == 0, lane == half)
    sine = jnp.logical_and(lane >= half, jnp.logical_not(lone))
    sign = jnp.where(sine, -1.0, 1.0)
    for strip in range(rows // TILE):
        at = slice(strip * TILE, (strip + 1) * TILE)
        xs = [recv1[r, at, :].astype(jnp.float32) for r in range(ways)]
        for a, (re, im) in enumerate(half_spectrum(xs)):
            im = jnp.zeros_like(re) if im is None else im
            top = jnp.where(sine, im, re).astype(jnp.bfloat16)
            low = jnp.where(sine, -re, im).astype(jnp.bfloat16)
            for t in range(pack):
                begin = t * rows + strip * TILE
                spec[a, begin : begin + TILE, :] = top[:, t * slots : (t + 1) * slots]
                begin += local_len
                spec[a, begin : begin + TILE, :] = low[:, t * slots : (t + 1) * slots]
    load_turn.wait()
    begin = 0
    for a in range(ways // 2 + 1):
        single = a == 0 or 2 * a == ways
        size = local_len if single else 2 * local_len
        made = jnp.dot(turn[begin : begin + size], spec[a], preferred_element_type=jnp.float32)
        begin += size
        for at, which in enumerate([a] if single else [a, ways - a]):
            piece = jnp.concatenate(
                [made[at * local_len + t * rows : at * local_len + (t + 1) * rows] for t in range(pack)], 1
            )
            outer[pl.ds(which, rows, stride=ways), :] = piece if at == 0 else piece * sign
    for r in range(ways):
        send2[r] = outer[r * rows : (r + 1) * rows, :].astype(jnp.bfloat16)
    copies2 = exchange(send2, recv2, 1)
    for count in range(3, steps):
        level(count)

    load_gather.wait()
    row_part = lax.broadcasted_iota(jnp.int32, (quads * LANES, GRP), 0) // slots % pack
    table = gather[...]
    table = jnp.concatenate(
        [jnp.where(row_part == t, table, jnp.zeros_like(table)) for t in range(pack)], 1
    )
    for copy in copies2:
        copy.wait_recv()
    columns = []
    for g in range(groups):
        left = jnp.concatenate([recv2[g * quads + quad] for quad in range(quads)], 1)
        made = jnp.dot(left, table, preferred_element_type=jnp.float32).astype(jnp.bfloat16)
        columns.append(
            jnp.concatenate([made[:, t * GRP : (t + 1) * GRP] for t in range(pack)], 0)
        )
    mixed = jnp.concatenate(columns, 1)
    level(steps)
    for _, get in fw_copies:
        get.wait_recv()

    mixed_v[...] = mixed
    for copy in copies1 + copies2 + pin_copies + list(ag_copies.values()):
        copy.wait_send()
    for put, _ in fw_copies:
        put.wait_send()


def output_map(chunk, mixed, wide, out_h, res, out_sem):
    stores = []
    for at in range(wide.shape[1] // chunk):
        span = slice(at * chunk, (at + 1) * chunk)
        res[:, span] = jnp.dot(
            mixed[...], wide[:, span], preferred_element_type=jnp.float32
        ).astype(jnp.bfloat16)
        copy = pltpu.make_async_copy(res.at[:, span], out_h.at[0, :, span], out_sem.at[at])
        copy.start()
        stores.append(copy)
    for copy in stores:
        copy.wait()


def fused(ways, cores, tokens, proj_in, proj_out):
    _, local_len, model = tokens.shape
    depth, features = proj_in.shape
    width = proj_out.shape[1]
    groups = features // GRP
    slots = features // ways
    pack = LANES // slots
    rows = local_len // pack
    consts = [jnp.asarray(t) for t in tables(ways, local_len, groups)]
    bf, f32 = jnp.bfloat16, jnp.float32
    dma = pltpu.SemaphoreType.DMA
    anywhere = pl.BlockSpec(memory_space=pltpu.HBM)
    mixed, wide = pl.pallas_call(
        functools.partial(kernel, ways, cores, groups),
        out_shape=(pltpu.VMEM((local_len, features), bf), pltpu.VMEM((features, model), bf)),
        in_specs=[anywhere] * 6,
        out_specs=(pl.BlockSpec(memory_space=pltpu.VMEM),) * 2,
        scratch_shapes=[
            pltpu.VMEM((cores, local_len, depth), bf),
            pltpu.VMEM((cores, depth, features), bf),
            pltpu.VMEM(consts[0].shape, bf),
            pltpu.VMEM(consts[1].shape, bf),
            pltpu.VMEM(consts[2].shape, bf),
            pltpu.VMEM((local_len, features), f32),
            pltpu.VMEM((ways, rows, LANES), bf),
            pltpu.VMEM((ways, rows, LANES), bf),
            pltpu.VMEM((ways // 2 + 1, 2 * local_len, slots), bf),
            pltpu.VMEM((ways * rows, LANES), f32),
            pltpu.VMEM((ways, rows, LANES), bf),
            pltpu.VMEM((ways, rows, LANES), bf),
            dma((cores + 5,)),
            dma((cores, PARTS)),
            dma((cores, PARTS)),
            dma((2, ways)),
            dma((2, ways)),
            dma((ways,)),
            dma((ways,)),
            dma((ways, cores)),
            dma((ways, cores)),
        ],
        compiler_params=pltpu.CompilerParams(
            collective_id=0, has_side_effects=True, vmem_limit_bytes=32 * 2**20
        ),
    )(*[pltpu.with_memory_space_constraint(x, pltpu.HBM) for x in (tokens, proj_in, proj_out, *consts)])
    chunk = 512
    return pl.pallas_call(
        functools.partial(output_map, chunk),
        out_shape=jax.ShapeDtypeStruct(tokens.shape, bf),
        in_specs=[pl.BlockSpec(memory_space=pltpu.VMEM)] * 2,
        out_specs=anywhere,
        scratch_shapes=[pltpu.VMEM((local_len, model), bf), dma((model // chunk,))],
        compiler_params=pltpu.CompilerParams(vmem_limit_bytes=16 * 2**20),
    )(mixed, wide)


def shards(ways, cores, tokens, proj_in, proj_out):
    _, local_len, model = tokens.shape
    depth, features = proj_in.shape
    width = proj_out.shape[1]
    groups = features // GRP
    slots = max(1, features // ways)
    pack = max(1, LANES // slots)
    fits = (
        ways >= 4
        and ways & (ways - 1) == 0
        and ways % groups == 0
        and slots * pack == LANES
        and slots % 2 == 0
        and cores == 2
        and local_len % pack == 0
        and (local_len // pack) % max(ways, TILE) == 0
        and width % LANES == 0
        and depth % (LANES * PARTS) == 0
        and model % 512 == 0
        and features % (cores * TILE) == 0
    )
    if fits:
        return fused(ways, cores, tokens, proj_in, proj_out)
    return plain(tokens, proj_in, proj_out)


def solution(mesh):
    in_specs = (P("col", "row", None), P("col", None), P(None, "row"))
    out_specs = P("col", "row", None)
    body = functools.partial(shards, mesh.shape["row"], mesh.shape["col"])
    return jax.shard_map(body, mesh=mesh, in_specs=in_specs, out_specs=out_specs, check_vma=False)
```
